32 devices in a mesh: grp: 2 (over y), ep: 4 (over z), tp: 4 (over x, core).
Axes of the slice: x: 2, y: 2, z: 4, core: 2. Of those that a mesh axis runs over, the one named last changes fastest.
Arguments:
- queries: bfloat16 [4096, 1024], P(('grp', 'ep'), 'tp'), parts along dimension 0, may hold values from -6 to 6
- key_rows: bfloat16 [4096, 512], P(('grp', 'ep'), 'tp'), parts along dimension 0, may hold values from -6 to 6
- value_rows: bfloat16 [4096, 512], P(('grp', 'ep'), 'tp'), parts along dimension 0, may hold values from -6 to 6
- query_gain: float32 [128], replicated, may hold values from 0.3 to 9
- key_gain: float32 [128], replicated, may hold values from 0.3 to 9
- log_forget: float32 [8, 4096], P('tp', 'grp'), parts along dimension 1, may hold values from -2048 to 0, as said below
- out_weight: bfloat16 [1024, 2048], P('tp'), may hold values from -0.1875 to 0.1875
- expert_rows: bfloat16 [4096, 2048], P(('grp', 'ep')), parts along dimension 0, may hold values from -6 to 6
- expert_gain: float32 [2048], replicated, may hold values from 0.1 to 1.9
- routes: int32 [2, 4096], P(None, ('grp', 'ep')), parts along dimension 1, may hold values from 0 to 31, as said below
- route_weight: float32 [2, 4096], P(None, ('grp', 'ep')), parts along dimension 1, may hold values from 0.1 to 1
- gate_weight: bfloat16 [32, 2048, 1024], P('ep', None, 'tp'), may hold values from -0.125 to 0.125
- up_weight: bfloat16 [32, 2048, 1024], P('ep', None, 'tp'), may hold values from -0.125 to 0.125
- down_weight: bfloat16 [32, 1024, 2048], P('ep', 'tp'), may hold values from -0.1875 to 0.1875
Outputs:
- mixer_out: bfloat16 [4096, 2048], P(('grp', 'ep', 'tp')), parts along dimension 0
- expert_out: bfloat16 [4096, 2048], P(('grp', 'ep'), 'tp'), parts along dimension 0
The draws below stay inside these ranges and needn't reach their ends.
There are 2 independent parts, one for each index of `grp`. The reference program is written for one: setup_inputs(seed, part) draws one part's arguments, and reference() takes and returns one part's arrays. A program takes and returns all parts, laid end to end along the dimension named above; an argument that names none is the same for every part. Nothing has to cross between parts.
Inputs may be any that keep to these rules, and one draw needn't show every extreme that they name: `log_forget`: each head's values never rise along the positions. `routes`: the 2 experts of a token differ and lie in one group of 8 consecutive numbers. Among the tokens of one index of ep (512 consecutive tokens), no expert is named more than 48 times, and in every draw some experts are named exactly 48 times in every such block.
All inputs are finite; a program needn't handle non-finite values.
Results may differ from the reference program's by a relative error of at most 0.012.
The reference program's roundings to bfloat16 on the way count: a program that leaves them out, or rounds other values in their place, can miss the bound.
Values may be sent and summed in bfloat16 or wider, within the bound.
A program may use at most 128 MiB of HBM per device.

```python
import math
import jax
import jax.numpy as jnp
from jax import lax

D = 2048
QUERY_HEADS = 8
KV_HEADS = 4
HEAD_SIZE = 128
EXPERTS = 32
GROUP_SIZE = 8
FF = 1024
TOP = 2
SPAN = 512
SEQUENCE_TOKENS = 2048
CAP = 48
N_EP = 4
N_TP = 4


def gain_draw(gain_key):
    return jnp.clip(1.0 + 0.18 * jax.random.normal(gain_key, (HEAD_SIZE,), jnp.float32), 0.3, 1.7)


def draw_query_gain(key, part):
    return gain_draw(jax.random.fold_in(key, 3))


def draw_key_gain(key, part):
    return gain_draw(jax.random.fold_in(key, 5))


def draw_log_forget(key, part):
    divided_keys = jax.random.split(jax.random.fold_in(key, 7), 7)
    token_position = jnp.arange(SEQUENCE_TOKENS, dtype=jnp.int32)
    shard_factor = jnp.exp(jax.random.uniform(divided_keys[0], (SEQUENCE_TOKENS // SPAN,), jnp.float32, -0.7, 0.7))
    factor_vector = jnp.repeat(shard_factor, SPAN)
    fast_rank = jax.random.permutation(divided_keys[1], QUERY_HEADS).astype(jnp.int32)
    is_fast = fast_rank < QUERY_HEADS // 2
    slow_rate = jax.random.uniform(divided_keys[2], (QUERY_HEADS,), jnp.float32, 0.3, 0.9) / SEQUENCE_TOKENS
    fast_rate = 1.0 / jax.random.uniform(divided_keys[3], (QUERY_HEADS,), jnp.float32, 30.0, 50.0)
    baseline_rate = jnp.where(is_fast, fast_rate, slow_rate)
    jitter_amount = jax.random.uniform(divided_keys[4], (QUERY_HEADS, SEQUENCE_TOKENS), jnp.float32, 0.5, 1.5)
    spike_position = jax.random.randint(divided_keys[5], (QUERY_HEADS, 3), 0, SEQUENCE_TOKENS)
    spike_length = -jnp.log(jax.random.uniform(divided_keys[6], (QUERY_HEADS, 3), jnp.float32, 0.6, 0.8))
    spike_events = jnp.sum(jnp.where(token_position[None, None, :] == spike_position[:, :, None], spike_length[:, :, None], 0.0), axis=1)
    logarithm_step = -(baseline_rate[:, None] * factor_vector[None, :] * jitter_amount + spike_events)
    return jnp.cumsum(logarithm_step, axis=1)


def route_block(block_key, full_group):
    divided_keys = jax.random.split(block_key, 4)
    full_rows = GROUP_SIZE * CAP // 2
    rest_rows = SPAN - full_rows
    other_sizes = jnp.array([rest_rows // 2, rest_rows // 3, rest_rows - rest_rows // 2 - rest_rows // 3], jnp.int32)
    others = (full_group + 1 + jax.random.permutation(divided_keys[0], 3).astype(jnp.int32)) % 4
    group_sizes = jnp.zeros((4,), jnp.int32).at[full_group].set(full_rows).at[others].set(other_sizes)
    group_ends = jnp.cumsum(group_sizes)
    token_position = jnp.arange(SPAN, dtype=jnp.int32)
    group_of = jnp.sum((token_position[:, None] >= group_ends[None, :]).astype(jnp.int32), axis=1)
    within = token_position - (group_ends - group_sizes)[group_of]
    orders = jax.vmap(lambda sub_key: jax.random.permutation(sub_key, GROUP_SIZE).astype(jnp.int32))(jax.random.split(divided_keys[1], 4))
    shifts = jax.random.randint(divided_keys[2], (4,), 0, GROUP_SIZE - 1)
    first_pick = orders[group_of, within % GROUP_SIZE]
    second_pick = orders[group_of, (within + 1 + (within // GROUP_SIZE + shifts[group_of]) % (GROUP_SIZE - 1)) % GROUP_SIZE]
    chosen = jnp.stack([group_of * GROUP_SIZE + first_pick, group_of * GROUP_SIZE + second_pick])
    shuffle = jax.random.permutation(divided_keys[3], SPAN)
    return chosen[:, shuffle]


def draw_routes(key, part):
    full_group = jax.random.randint(jax.random.fold_in(key, 11), (), 0, 4)
    block_keys = jax.random.split(jax.random.fold_in(key, 12), SEQUENCE_TOKENS // SPAN)
    blocks = jax.vmap(lambda block_key: route_block(block_key, full_group))(block_keys)
    return jnp.transpose(blocks, (1, 0, 2)).reshape(2, SEQUENCE_TOKENS).astype(jnp.int32)


def steps_of(key, dims, cuts, smallest, high):
    def one(position, parts):
        draws = jax.random.uniform(jax.random.fold_in(jax.random.fold_in(key, 6), position), (parts,), jnp.float32, smallest / len(cuts), high / len(cuts))
        return jnp.repeat(jnp.exp(draws), dims[position] // parts).reshape((-1,) + (1,) * (len(dims) - position - 1))

    factor_of = one(*cuts[0])
    for cut in cuts[1:]:
        factor_of = factor_of * one(*cut)
    return factor_of


def noise(rng, shape, spread, bound, cuts=(), held_as=jnp.bfloat16):
    result = jax.random.normal(rng, shape, jnp.float32) * spread
    if len(cuts) > 0:
        result = steps_of(rng, shape, cuts, -0.22, 0.18) * result
    return jnp.clip(result, min=-bound, max=bound).astype(held_as)


def setup_inputs(seed: int = 0, part: int = 0) -> dict:
    keys = jax.random.split(jax.random.key(seed), 15)
    part_keys = jax.random.split(jax.random.fold_in(keys[14], part), 15)
    return {
        "queries": noise(part_keys[0], (SEQUENCE_TOKENS, QUERY_HEADS * HEAD_SIZE), 1.0, 6.0, ((0, 4), (1, 4))),
        "key_rows": noise(part_keys[1], (SEQUENCE_TOKENS, KV_HEADS * HEAD_SIZE), 1.0, 6.0, ((0, 4), (1, 4))),
        "value_rows": noise(part_keys[2], (SEQUENCE_TOKENS, KV_HEADS * HEAD_SIZE), 1.0, 6.0, ((0, 4), (1, 4))),
        "query_gain": draw_query_gain(jax.random.fold_in(keys[14], 71), part),
        "key_gain": draw_key_gain(jax.random.fold_in(keys[14], 71), part),
        "log_forget": draw_log_forget(jax.random.fold_in(jax.random.fold_in(keys[14], part), 71), part),
        "out_weight": noise(keys[6], (QUERY_HEADS * HEAD_SIZE, D), (QUERY_HEADS * HEAD_SIZE) ** -0.5, 0.1875, ((0, 4),)),
        "expert_rows": noise(part_keys[7], (SEQUENCE_TOKENS, D), 1.0, 6.0, ((0, 4),)),
        "expert_gain": jnp.clip(1.0 + 0.18 * jax.random.normal(keys[8], (D,), jnp.float32), 0.1, 1.9),
        "routes": draw_routes(jax.random.fold_in(jax.random.fold_in(keys[14], part), 71), part),
        "route_weight": jnp.clip(jnp.exp(math.log(1.0) - 2.3025851 * jax.random.uniform(part_keys[10], (TOP, SEQUENCE_TOKENS), jnp.float32) ** steps_of(part_keys[10], (TOP, SEQUENCE_TOKENS), ((1, 4),), -0.2, 0.2)), 0.1, 1.0),
        "gate_weight": noise(keys[11], (EXPERTS, D, FF), D ** -0.5, 0.125, ((0, 4), (2, 4))),
        "up_weight": noise(keys[12], (EXPERTS, D, FF), D ** -0.5, 0.125, ((0, 4), (2, 4))),
        "down_weight": noise(keys[13], (EXPERTS, FF, D), FF ** -0.5, 0.1875, ((0, 4), (1, 4))),
    }


def head_norm(inputs, scale_gain):
    widened = inputs.astype(jnp.float32)
    factor = lax.rsqrt(lax.optimization_barrier(jnp.mean(widened * widened, axis=-1, keepdims=True)) + 1e-06)
    return widened * factor * scale_gain.astype(jnp.float32)

def slot_table(chosen, experts_all, capacity):
    n_rows = chosen.shape[0]
    per_row = chosen.shape[1]
    flat_ids = chosen.reshape(-1)
    one_hot = (flat_ids[:, None] == jnp.arange(experts_all, dtype=jnp.int32)[None, :]).astype(jnp.int32)
    within = lax.optimization_barrier(jnp.sum((jnp.cumsum(one_hot, axis=0) - 1) * one_hot, axis=1))
    slot_index = (flat_ids * capacity + within).astype(jnp.int32)
    row_of = jnp.arange(n_rows * per_row, dtype=jnp.int32) // per_row
    slot_owner = jnp.full((experts_all * capacity,), n_rows, jnp.int32).at[slot_index].set(row_of)
    return (slot_index.reshape(n_rows, per_row), slot_owner)

def reference(queries, key_rows, value_rows, query_gain, key_gain, log_forget, out_weight, expert_rows, expert_gain, routes, route_weight, gate_weight, up_weight, down_weight):
    span_len = SEQUENCE_TOKENS // N_EP
    group_ratio = QUERY_HEADS // KV_HEADS
    scale_qk = HEAD_SIZE ** (-0.5)
    q_all = lax.optimization_barrier(head_norm(queries.reshape(SEQUENCE_TOKENS, KV_HEADS, group_ratio, HEAD_SIZE), query_gain).astype(jnp.bfloat16)).astype(jnp.float32)
    k_all = lax.optimization_barrier(head_norm(key_rows.reshape(SEQUENCE_TOKENS, KV_HEADS, HEAD_SIZE), key_gain).astype(jnp.bfloat16)).astype(jnp.float32)
    v_all = value_rows.reshape(SEQUENCE_TOKENS, KV_HEADS, HEAD_SIZE).astype(jnp.float32)
    positions = jnp.arange(span_len, dtype=jnp.int32)

    def query_block(block_index):
        q_here = lax.dynamic_slice_in_dim(q_all, block_index * span_len, span_len, 0)
        gates_here = lax.dynamic_slice_in_dim(log_forget, block_index * span_len, span_len, 1)
        gates_here = gates_here.T.reshape(span_len, KV_HEADS, group_ratio)

        def key_step(key_index, running):
            run_max, run_sum, run_acc = running
            k_here = lax.dynamic_slice_in_dim(k_all, key_index * span_len, span_len, 0)
            v_here = lax.dynamic_slice_in_dim(v_all, key_index * span_len, span_len, 0)
            key_gates = lax.dynamic_slice_in_dim(log_forget, key_index * span_len, span_len, 1)
            key_gates = key_gates.reshape(KV_HEADS, group_ratio, span_len)
            scores = jnp.einsum('qgrd,kgd->qgrk', q_here, k_here) * scale_qk
            scores = scores + gates_here[..., None] - key_gates[None]
            visible = (key_index * span_len + positions)[None, :] <= (block_index * span_len + positions)[:, None]
            scores = jnp.where(visible[:, None, None, :], scores, -jnp.inf)
            new_max = jnp.maximum(run_max, lax.optimization_barrier(jnp.max(scores, axis=-1)))
            shrink = jnp.exp(run_max - new_max)
            weights = jnp.exp(scores - new_max[..., None])
            run_sum = shrink * run_sum + lax.optimization_barrier(jnp.sum(weights, axis=-1))
            weights_low = lax.optimization_barrier(weights.astype(jnp.bfloat16)).astype(jnp.float32)
            gathered = jnp.einsum('qgrk,kgd->qgrd', weights_low, v_here)
            return (new_max, run_sum, shrink[..., None] * run_acc + gathered)
        start_state = (jnp.full((span_len, KV_HEADS, group_ratio), -jnp.inf, jnp.float32), jnp.zeros((span_len, KV_HEADS, group_ratio), jnp.float32), jnp.zeros((span_len, KV_HEADS, group_ratio, HEAD_SIZE), jnp.float32))
        run_max, run_sum, run_acc = lax.fori_loop(0, block_index + 1, key_step, start_state)
        return (run_acc / run_sum[..., None]).astype(jnp.bfloat16)
    attended = lax.map(query_block, jnp.arange(N_EP, dtype=jnp.int32))
    attended = attended.reshape(SEQUENCE_TOKENS, QUERY_HEADS * HEAD_SIZE)
    mixer_out = jnp.dot(attended, out_weight, preferred_element_type=jnp.float32).astype(jnp.bfloat16)
    normed = head_norm(expert_rows, expert_gain).astype(jnp.bfloat16)
    block_routes = routes.reshape(TOP, N_EP, span_len).transpose(1, 2, 0)
    slot_all, owner_all = jax.vmap(lambda chosen: slot_table(chosen, EXPERTS, CAP))(block_routes)
    block_base = jnp.arange(N_EP, dtype=jnp.int32)[:, None] * span_len
    global_rows = jnp.where(owner_all == span_len, SEQUENCE_TOKENS, owner_all + block_base).astype(jnp.int32)
    row_index = global_rows.reshape(N_EP, EXPERTS, CAP).transpose(1, 0, 2).reshape(EXPERTS, N_EP * CAP)
    padded = jnp.concatenate([normed, jnp.zeros((1, D), jnp.bfloat16)], axis=0)
    ff_part = FF // N_TP

    def one_expert(inputs):
        index_rows, w_gate, w_up, w_down = inputs
        taken = padded[index_rows]
        gate_part = jnp.dot(taken, w_gate, preferred_element_type=jnp.float32)
        up_part = jnp.dot(taken, w_up, preferred_element_type=jnp.float32)
        hidden = (jax.nn.silu(gate_part) * up_part).astype(jnp.bfloat16)
        running = jnp.zeros((N_EP * CAP, D), jnp.float32)
        for part_index in range(N_TP):
            piece = jnp.dot(hidden[:, part_index * ff_part:(part_index + 1) * ff_part], w_down[part_index * ff_part:(part_index + 1) * ff_part], preferred_element_type=jnp.float32)
            running = running + lax.optimization_barrier(piece.astype(jnp.bfloat16)).astype(jnp.float32)
        return running.astype(jnp.bfloat16)
    results = lax.map(one_expert, (row_index, gate_weight, up_weight, down_weight))
    result_table = results.reshape(EXPERTS, N_EP, CAP, D)
    expert_of = slot_all // CAP
    cell_of = slot_all % CAP
    block_id = jnp.arange(N_EP, dtype=jnp.int32)[:, None, None]
    picked = result_table[expert_of, block_id, cell_of]
    weights_all = route_weight.reshape(TOP, N_EP, span_len).transpose(1, 2, 0)
    expert_out = lax.optimization_barrier(jnp.sum(picked.astype(jnp.float32) * weights_all[..., None], axis=2))
    expert_out = expert_out.astype(jnp.bfloat16).reshape(SEQUENCE_TOKENS, D)
    return (mixer_out, expert_out)
```

```python
import jax
import jax.numpy as jnp
from jax import lax
from jax.sharding import PartitionSpec as P

HEAD_SIZE = 128
EXPERTS = 32
TOP = 2
GROUP_SIZE = 8
META = 128


def head_norm(inputs, scale_gain):
    widened = inputs.astype(jnp.float32)
    factor = lax.rsqrt(jnp.mean(widened * widened, axis=-1, keepdims=True) + 1e-06)
    return widened * factor * scale_gain


def slot_table(chosen, experts_all, capacity):
    n_rows = chosen.shape[0]
    per_row = chosen.shape[1]
    flat_ids = chosen.reshape(-1)
    one_hot = (flat_ids[:, None] == jnp.arange(experts_all, dtype=jnp.int32)[None, :]).astype(
        jnp.int32
    )
    within = jnp.sum((jnp.cumsum(one_hot, axis=0) - 1) * one_hot, axis=1)
    slot_index = flat_ids * capacity + within
    row_of = jnp.arange(n_rows * per_row, dtype=jnp.int32) // per_row
    slot_owner = jnp.full((experts_all * capacity,), n_rows, jnp.int32).at[slot_index].set(row_of)
    return (slot_index.reshape(n_rows, per_row), slot_owner)


def mixer_half(queries, key_rows, value_rows, query_gain, key_gain, log_forget, out_weight):
    span_rows = queries.shape[0]
    heads_dev = queries.shape[1] // HEAD_SIZE
    kv_dev = key_rows.shape[1] // HEAD_SIZE
    group_ratio = heads_dev // kv_dev
    scale_qk = HEAD_SIZE ** (-0.5)
    q_normed = head_norm(
        queries.reshape(span_rows, kv_dev, group_ratio, HEAD_SIZE), query_gain
    ).astype(jnp.bfloat16)
    k_normed = head_norm(key_rows.reshape(span_rows, kv_dev, HEAD_SIZE), key_gain).astype(
        jnp.bfloat16
    )
    key_value = jnp.concatenate(
        [k_normed.reshape(span_rows, kv_dev * HEAD_SIZE), value_rows], axis=1
    )
    first_row = lax.axis_index("ep") * span_rows
    last_row = first_row + span_rows - 1
    query_pos = first_row + jnp.arange(span_rows, dtype=jnp.int32)
    query_gates = lax.dynamic_slice_in_dim(log_forget, first_row, span_rows, 1)
    query_gates = query_gates.T.reshape(span_rows, kv_dev, group_ratio)

    def add_block(running, kv_block, key_start):
        run_max, run_sum, run_acc = running
        block_len = kv_block.shape[0]
        k_block = kv_block[:, : kv_dev * HEAD_SIZE].reshape(block_len, kv_dev, HEAD_SIZE)
        v_block = kv_block[:, kv_dev * HEAD_SIZE :].reshape(block_len, kv_dev, HEAD_SIZE)
        key_gates = lax.dynamic_slice_in_dim(log_forget, key_start, block_len, 1)
        key_gates = key_gates.reshape(kv_dev, group_ratio, block_len)
        scores = (
            jnp.einsum("qgrd,kgd->qgrk", q_normed, k_block, preferred_element_type=jnp.float32)
            * scale_qk
        )
        scores = scores + query_gates[..., None] - key_gates[None]
        key_pos = key_start + jnp.arange(block_len, dtype=jnp.int32)
        visible = key_pos[None, :] <= query_pos[:, None]
        scores = jnp.where(visible[:, None, None, :], scores, -jnp.inf)
        new_max = jnp.maximum(run_max, jnp.max(scores, axis=-1))
        shrink = jnp.exp(run_max - new_max)
        weights = jnp.exp(scores - new_max[..., None])
        run_sum = shrink * run_sum + jnp.sum(weights, axis=-1)
        gathered = jnp.einsum(
            "qgrk,kgd->qgrd",
            weights.astype(jnp.bfloat16),
            v_block,
            preferred_element_type=jnp.float32,
        )
        return (new_max, run_sum, shrink[..., None] * run_acc + gathered)

    start_state = (
        jnp.full((span_rows, kv_dev, group_ratio), -jnp.inf, jnp.float32),
        jnp.zeros((span_rows, kv_dev, group_ratio), jnp.float32),
        jnp.zeros((span_rows, kv_dev, group_ratio, HEAD_SIZE), jnp.float32),
    )
    kv_piece = lax.all_gather(key_value, "ep", axis=0, tiled=True)
    block_len = min(kv_piece.shape[0], span_rows)
    n_blocks = kv_piece.shape[0] // block_len

    def one_block(block_number, running_in):
        key_start = block_number * block_len
        kv_block = lax.dynamic_slice_in_dim(kv_piece, block_number * block_len, block_len, 0)

        def take_block(running_now):
            return add_block(running_now, kv_block, key_start)

        def skip_block(running_now):
            return running_now

        return lax.cond(key_start <= last_row, take_block, skip_block, running_in)

    run_max, run_sum, run_acc = lax.fori_loop(0, n_blocks, one_block, start_state)
    attended = (
        (run_acc / run_sum[..., None])
        .astype(jnp.bfloat16)
        .reshape(span_rows, heads_dev * HEAD_SIZE)
    )
    return lax.psum_scatter(
        jnp.dot(attended, out_weight, preferred_element_type=jnp.float32).astype(jnp.bfloat16),
        "tp",
        scatter_dimension=0,
        tiled=True,
    )


def experts_half(
    expert_rows, expert_gain, routes, route_weight, gate_weight, up_weight, down_weight
):
    n_tp = lax.axis_size("tp")
    n_ep = lax.axis_size("ep")
    span_rows = expert_rows.shape[0]
    model_width = expert_rows.shape[1]
    exp_dev = gate_weight.shape[0]
    capacity = n_tp * ((3 * (span_rows // n_tp) * TOP + 2 * EXPERTS - 1) // (2 * EXPERTS))
    normed = head_norm(expert_rows, expert_gain).astype(jnp.bfloat16)
    slot_index, slot_owner = slot_table(routes.T, EXPERTS, capacity)
    padded = jnp.concatenate([normed, jnp.zeros((1, model_width), jnp.bfloat16)], axis=0)
    part_len = capacity // n_tp
    owner_part = lax.dynamic_slice_in_dim(
        slot_owner.reshape(EXPERTS, capacity), lax.axis_index("tp") * part_len, part_len, 1
    )
    send_rows = padded[owner_part].reshape(n_ep, exp_dev, part_len, model_width)
    arrived = lax.all_to_all(send_rows, "ep", split_axis=0, concat_axis=0, tiled=True)
    slot_rows = lax.all_gather(arrived, "tp", axis=2, tiled=True)
    gate_part = jnp.einsum(
        "nxcd,xdf->nxcf", slot_rows, gate_weight, preferred_element_type=jnp.float32
    )
    up_part = jnp.einsum("nxcd,xdf->nxcf", slot_rows, up_weight, preferred_element_type=jnp.float32)
    hidden = (jax.nn.silu(gate_part) * up_part).astype(jnp.bfloat16)
    partial_out = jnp.einsum(
        "nxcf,xfd->nxcd", hidden, down_weight, preferred_element_type=jnp.float32
    )
    summed = lax.psum_scatter(
        partial_out.astype(jnp.bfloat16), "tp", scatter_dimension=3, tiled=True
    )
    returned = lax.all_to_all(summed, "ep", split_axis=0, concat_axis=0, tiled=True)
    result_table = returned.reshape(EXPERTS * capacity, returned.shape[3])
    picked = result_table[slot_index]
    combined = jnp.sum(picked.astype(jnp.float32) * route_weight.T[..., None], axis=1)
    return combined.astype(jnp.bfloat16)

def route_plan(routes, route_weight, n_dest, exp_dev, row_cap):
    span_rows = routes.shape[1]
    picks = routes[:, :, None] == jnp.arange(EXPERTS, dtype=jnp.int32)
    dest = routes[0] // exp_dev
    to_dest = dest[:, None] == jnp.arange(n_dest, dtype=jnp.int32)
    marks = jnp.concatenate([picks[0] | picks[1], to_dest], axis=1).astype(jnp.bfloat16)
    tokens = jnp.arange(span_rows, dtype=jnp.int32)
    earlier = (tokens[None, :] < tokens[:, None]).astype(jnp.bfloat16)
    ahead = jnp.dot(earlier, marks, preferred_element_type=jnp.float32)
    rank = jnp.sum(jnp.where(to_dest, ahead[:, EXPERTS:], 0.0), axis=1)
    columns = []
    for j in range(TOP):
        within = jnp.sum(jnp.where(picks[j], ahead[:, :EXPERTS], 0.0), axis=1)
        columns += [(routes[j] % exp_dev + 1).astype(jnp.float32), within]
    for j in range(TOP):
        high = lax.reduce_precision(route_weight[j], 8, 7)
        columns += [high, route_weight[j] - high]
    meta = jnp.pad(jnp.stack(columns, axis=1), ((0, 0), (0, META - len(columns))))
    return dest * row_cap + rank.astype(jnp.int32), meta.astype(jnp.bfloat16)


def spread_rows(send_rows):
    arrived = lax.all_to_all(send_rows, "ep", split_axis=0, concat_axis=0, tiled=True)
    return lax.all_gather(arrived, "tp", axis=1, tiled=True)


def return_rows(partial_rows):
    summed = lax.psum_scatter(partial_rows, "tp", scatter_dimension=2, tiled=True)
    return lax.all_to_all(summed, "ep", split_axis=0, concat_axis=0, tiled=True)


def grouped_experts_half(
    expert_rows, expert_gain, routes, route_weight, gate_weight, up_weight, down_weight
):
    n_tp = lax.axis_size("tp")
    n_ep = lax.axis_size("ep")
    span_rows, model_width = expert_rows.shape
    exp_dev = gate_weight.shape[0]
    capacity = n_tp * ((3 * (span_rows // n_tp) * TOP + 2 * EXPERTS - 1) // (2 * EXPERTS))
    row_cap = exp_dev * capacity // TOP
    part_len = row_cap // n_tp
    row_of, meta = route_plan(routes, route_weight, n_ep, exp_dev, row_cap)
    normed = head_norm(expert_rows, expert_gain).astype(jnp.bfloat16)
    wanted = jnp.arange(n_ep, dtype=jnp.int32)[:, None] * row_cap + (
        lax.axis_index("tp") * part_len + jnp.arange(part_len, dtype=jnp.int32)
    )
    select = (wanted.reshape(-1)[:, None] == row_of[None, :]).astype(jnp.bfloat16)
    send_rows = jnp.dot(
        select, jnp.concatenate([normed, meta], axis=1), preferred_element_type=jnp.float32
    ).astype(jnp.bfloat16)
    arrived = spread_rows(send_rows.reshape(n_ep, part_len, model_width + META))
    notes = arrived[:, :, model_width : model_width + 8].astype(jnp.float32)
    slots = jnp.arange(exp_dev * capacity, dtype=jnp.float32)
    hits = []
    for j in range(TOP):
        local = notes[:, :, 2 * j]
        slot = jnp.where(local > 0, (local - 1) * capacity + notes[:, :, 2 * j + 1], -1.0)
        hits.append(slot[:, :, None] == slots)
    slot_rows = jnp.einsum(
        "nrq,nrd->nqd",
        (hits[0] | hits[1]).astype(jnp.bfloat16),
        arrived[:, :, :model_width],
        preferred_element_type=jnp.float32,
    ).astype(jnp.bfloat16)
    slot_rows = slot_rows.reshape(n_ep, exp_dev, capacity, model_width)
    gate_part = jnp.einsum(
        "nxcd,xdf->nxcf", slot_rows, gate_weight, preferred_element_type=jnp.float32
    )
    up_part = jnp.einsum("nxcd,xdf->nxcf", slot_rows, up_weight, preferred_element_type=jnp.float32)
    hidden = (jax.nn.silu(gate_part) * up_part).astype(jnp.bfloat16)
    down_part = jnp.einsum(
        "nxcf,xfd->nxcd", hidden, down_weight, preferred_element_type=jnp.float32
    ).astype(jnp.bfloat16)
    down_part = down_part.reshape(n_ep, exp_dev * capacity, model_width)
    partial_rows = 0.0
    for piece in range(2):
        weights = sum(
            jnp.where(hits[j], notes[:, :, 2 * TOP + 2 * j + piece][:, :, None], 0.0)
            for j in range(TOP)
        )
        partial_rows = partial_rows + jnp.einsum(
            "nrq,nqd->nrd",
            weights.astype(jnp.bfloat16),
            down_part,
            preferred_element_type=jnp.float32,
        )
    returned = return_rows(partial_rows.astype(jnp.bfloat16))
    returned = returned.reshape(n_ep * row_cap, model_width // n_tp)
    all_rows = jnp.arange(n_ep * row_cap, dtype=jnp.int32)
    return jnp.dot(
        (row_of[:, None] == all_rows[None, :]).astype(jnp.bfloat16),
        returned,
        preferred_element_type=jnp.float32,
    ).astype(jnp.bfloat16)


def on_device(
    queries,
    key_rows,
    value_rows,
    query_gain,
    key_gain,
    log_forget,
    out_weight,
    expert_rows,
    expert_gain,
    routes,
    route_weight,
    gate_weight,
    up_weight,
    down_weight,
):
    mixer_out = mixer_half(
        queries, key_rows, value_rows, query_gain, key_gain, log_forget, out_weight
    )
    whole_groups = gate_weight.shape[0] % GROUP_SIZE == 0
    run_experts = grouped_experts_half if whole_groups else experts_half
    expert_out = run_experts(
        expert_rows, expert_gain, routes, route_weight, gate_weight, up_weight, down_weight
    )
    return (mixer_out, expert_out)


def solution(mesh):
    in_specs = (
        P(("grp", "ep"), "tp"),
        P(("grp", "ep"), "tp"),
        P(("grp", "ep"), "tp"),
        P(),
        P(),
        P("tp", "grp"),
        P("tp", None),
        P(("grp", "ep"), None),
        P(),
        P(None, ("grp", "ep")),
        P(None, ("grp", "ep")),
        P("ep", None, "tp"),
        P("ep", None, "tp"),
        P("ep", "tp", None),
    )
    out_specs = (P(("grp", "ep", "tp"), None), P(("grp", "ep"), "tp"))
    return jax.shard_map(
        on_device, mesh=mesh, in_specs=in_specs, out_specs=out_specs, check_vma=False
    )
```

```python
import functools

import jax
import jax.numpy as jnp
from jax import lax
from jax.experimental import pallas as pl
from jax.experimental.pallas import tpu as pltpu
from jax.sharding import PartitionSpec as P

HEAD_SIZE = 128
EXPERTS = 32
TOP = 2
GROUP_SIZE = 8
META = 128


def head_norm(inputs, scale_gain):
    widened = inputs.astype(jnp.float32)
    factor = lax.rsqrt(jnp.mean(widened * widened, axis=-1, keepdims=True) + 1e-06)
    return widened * factor * scale_gain


def slot_table(chosen, experts_all, capacity):
    n_rows = chosen.shape[0]
    per_row = chosen.shape[1]
    flat_ids = chosen.reshape(-1)
    one_hot = (flat_ids[:, None] == jnp.arange(experts_all, dtype=jnp.int32)[None, :]).astype(
        jnp.int32
    )
    within = jnp.sum((jnp.cumsum(one_hot, axis=0) - 1) * one_hot, axis=1)
    slot_index = flat_ids * capacity + within
    row_of = jnp.arange(n_rows * per_row, dtype=jnp.int32) // per_row
    slot_owner = jnp.full((experts_all * capacity,), n_rows, jnp.int32).at[slot_index].set(row_of)
    return (slot_index.reshape(n_rows, per_row), slot_owner)


def mixer_half(queries, key_rows, value_rows, query_gain, key_gain, log_forget, out_weight):
    span_rows = queries.shape[0]
    heads_dev = queries.shape[1] // HEAD_SIZE
    kv_dev = key_rows.shape[1] // HEAD_SIZE
    group_ratio = heads_dev // kv_dev
    scale_qk = HEAD_SIZE ** (-0.5)
    q_normed = head_norm(
        queries.reshape(span_rows, kv_dev, group_ratio, HEAD_SIZE), query_gain
    ).astype(jnp.bfloat16)
    k_normed = head_norm(key_rows.reshape(span_rows, kv_dev, HEAD_SIZE), key_gain).astype(
        jnp.bfloat16
    )
    key_value = jnp.concatenate(
        [k_normed.reshape(span_rows, kv_dev * HEAD_SIZE), value_rows], axis=1
    )
    first_row = lax.axis_index("ep") * span_rows
    last_row = first_row + span_rows - 1
    query_pos = first_row + jnp.arange(span_rows, dtype=jnp.int32)
    query_gates = lax.dynamic_slice_in_dim(log_forget, first_row, span_rows, 1)
    query_gates = query_gates.T.reshape(span_rows, kv_dev, group_ratio)

    def add_block(running, kv_block, key_start):
        run_max, run_sum, run_acc = running
        block_len = kv_block.shape[0]
        k_block = kv_block[:, : kv_dev * HEAD_SIZE].reshape(block_len, kv_dev, HEAD_SIZE)
        v_block = kv_block[:, kv_dev * HEAD_SIZE :].reshape(block_len, kv_dev, HEAD_SIZE)
        key_gates = lax.dynamic_slice_in_dim(log_forget, key_start, block_len, 1)
        key_gates = key_gates.reshape(kv_dev, group_ratio, block_len)
        scores = (
            jnp.einsum("qgrd,kgd->qgrk", q_normed, k_block, preferred_element_type=jnp.float32)
            * scale_qk
        )
        scores = scores + query_gates[..., None] - key_gates[None]
        key_pos = key_start + jnp.arange(block_len, dtype=jnp.int32)
        visible = key_pos[None, :] <= query_pos[:, None]
        scores = jnp.where(visible[:, None, None, :], scores, -jnp.inf)
        new_max = jnp.maximum(run_max, jnp.max(scores, axis=-1))
        shrink = jnp.exp(run_max - new_max)
        weights = jnp.exp(scores - new_max[..., None])
        run_sum = shrink * run_sum + jnp.sum(weights, axis=-1)
        gathered = jnp.einsum(
            "qgrk,kgd->qgrd",
            weights.astype(jnp.bfloat16),
            v_block,
            preferred_element_type=jnp.float32,
        )
        return (new_max, run_sum, shrink[..., None] * run_acc + gathered)

    start_state = (
        jnp.full((span_rows, kv_dev, group_ratio), -jnp.inf, jnp.float32),
        jnp.zeros((span_rows, kv_dev, group_ratio), jnp.float32),
        jnp.zeros((span_rows, kv_dev, group_ratio, HEAD_SIZE), jnp.float32),
    )
    kv_piece = lax.all_gather(key_value, "ep", axis=0, tiled=True)
    block_len = min(kv_piece.shape[0], span_rows)
    n_blocks = kv_piece.shape[0] // block_len

    def one_block(block_number, running_in):
        key_start = block_number * block_len
        kv_block = lax.dynamic_slice_in_dim(kv_piece, block_number * block_len, block_len, 0)

        def take_block(running_now):
            return add_block(running_now, kv_block, key_start)

        def skip_block(running_now):
            return running_now

        return lax.cond(key_start <= last_row, take_block, skip_block, running_in)

    run_max, run_sum, run_acc = lax.fori_loop(0, n_blocks, one_block, start_state)
    attended = (
        (run_acc / run_sum[..., None])
        .astype(jnp.bfloat16)
        .reshape(span_rows, heads_dev * HEAD_SIZE)
    )
    return jnp.dot(attended, out_weight, preferred_element_type=jnp.float32).astype(jnp.bfloat16)


def experts_half(
    expert_rows, expert_gain, routes, route_weight, gate_weight, up_weight, down_weight
):
    n_tp = lax.axis_size("tp")
    n_ep = lax.axis_size("ep")
    span_rows = expert_rows.shape[0]
    model_width = expert_rows.shape[1]
    exp_dev = gate_weight.shape[0]
    capacity = n_tp * ((3 * (span_rows // n_tp) * TOP + 2 * EXPERTS - 1) // (2 * EXPERTS))
    normed = head_norm(expert_rows, expert_gain).astype(jnp.bfloat16)
    slot_index, slot_owner = slot_table(routes.T, EXPERTS, capacity)
    padded = jnp.concatenate([normed, jnp.zeros((1, model_width), jnp.bfloat16)], axis=0)
    part_len = capacity // n_tp
    owner_part = lax.dynamic_slice_in_dim(
        slot_owner.reshape(EXPERTS, capacity), lax.axis_index("tp") * part_len, part_len, 1
    )
    send_rows = padded[owner_part].reshape(n_ep, exp_dev, part_len, model_width)
    arrived = lax.all_to_all(send_rows, "ep", split_axis=0, concat_axis=0, tiled=True)
    slot_rows = lax.all_gather(arrived, "tp", axis=2, tiled=True)
    gate_part = jnp.einsum(
        "nxcd,xdf->nxcf", slot_rows, gate_weight, preferred_element_type=jnp.float32
    )
    up_part = jnp.einsum("nxcd,xdf->nxcf", slot_rows, up_weight, preferred_element_type=jnp.float32)
    hidden = (jax.nn.silu(gate_part) * up_part).astype(jnp.bfloat16)
    partial_out = jnp.einsum(
        "nxcf,xfd->nxcd", hidden, down_weight, preferred_element_type=jnp.float32
    )
    summed = lax.psum_scatter(
        partial_out.astype(jnp.bfloat16), "tp", scatter_dimension=3, tiled=True
    )
    returned = lax.all_to_all(summed, "ep", split_axis=0, concat_axis=0, tiled=True)
    result_table = returned.reshape(EXPERTS * capacity, returned.shape[3])
    picked = result_table[slot_index]
    combined = jnp.sum(picked.astype(jnp.float32) * route_weight.T[..., None], axis=1)
    return combined.astype(jnp.bfloat16)

def route_plan(routes, route_weight, n_dest, exp_dev, row_cap):
    span_rows = routes.shape[1]
    picks = routes[:, :, None] == jnp.arange(EXPERTS, dtype=jnp.int32)
    dest = routes[0] // exp_dev
    to_dest = dest[:, None] == jnp.arange(n_dest, dtype=jnp.int32)
    marks = jnp.concatenate([picks[0] | picks[1], to_dest], axis=1).astype(jnp.bfloat16)
    tokens = jnp.arange(span_rows, dtype=jnp.int32)
    earlier = (tokens[None, :] < tokens[:, None]).astype(jnp.bfloat16)
    ahead = jnp.dot(earlier, marks, preferred_element_type=jnp.float32)
    rank = jnp.sum(jnp.where(to_dest, ahead[:, EXPERTS:], 0.0), axis=1)
    columns = []
    for j in range(TOP):
        within = jnp.sum(jnp.where(picks[j], ahead[:, :EXPERTS], 0.0), axis=1)
        columns += [(routes[j] % exp_dev + 1).astype(jnp.float32), within]
    for j in range(TOP):
        high = lax.reduce_precision(route_weight[j], 8, 7)
        columns += [high, route_weight[j] - high]
    meta = jnp.pad(jnp.stack(columns, axis=1), ((0, 0), (0, META - len(columns))))
    return dest * row_cap + rank.astype(jnp.int32), meta.astype(jnp.bfloat16)


def ring_peers(n_ep, n_tp):
    me = lax.axis_index("ep")
    mine = lax.axis_index("tp")
    pair = mine + 1 - 2 * (mine % 2)
    across = (mine + n_tp // 2) % n_tp
    return me, mine, pair, across


def meet(me, pair, across, n_ep):
    barrier = pltpu.get_barrier_semaphore()
    peers = [{"ep": (me + k) % n_ep} for k in range(1, n_ep)] + [{"tp": pair}, {"tp": across}]
    for peer in peers:
        pl.semaphore_signal(
            barrier, inc=1, device_id=peer, device_id_type=pl.DeviceIdType.MESH
        )
    pl.semaphore_wait(barrier, len(peers))


def remote(src, dst, send_sem, recv_sem, peer):
    return pltpu.make_async_remote_copy(
        src_ref=src,
        dst_ref=dst,
        send_sem=send_sem,
        recv_sem=recv_sem,
        device_id=peer,
        device_id_type=pl.DeviceIdType.MESH,
    )


def spread_kernel(
    n_ep, n_tp, send_ref, out_ref, own_sem, z_send, z_recv, x_send, x_recv, c_send, c_recv
):
    me, mine, pair, across = ring_peers(n_ep, n_tp)
    meet(me, pair, across, n_ep)
    along = []
    for k in range(1, n_ep):
        dest = (me + k) % n_ep
        copy = remote(
            send_ref.at[dest], out_ref.at[me, mine], z_send.at[k], z_recv.at[k], {"ep": dest}
        )
        copy.start()
        along.append(copy)
    own = pltpu.make_async_copy(send_ref.at[me], out_ref.at[me, mine], own_sem)
    own.start()
    crossing = []
    pairing = []

    def pass_on(k):
        source = (me + n_ep - k) % n_ep
        block = send_ref.at[me] if k == 0 else out_ref.at[source, mine]
        place = out_ref.at[source, mine]
        copy = remote(block, place, x_send.at[k], x_recv.at[k], {"tp": across})
        copy.start()
        crossing.append(copy)
        copy = remote(block, place, c_send.at[0, k], c_recv.at[0, k], {"tp": pair})
        copy.start()
        pairing.append(copy)

    def relay(k):
        source = (me + n_ep - k) % n_ep
        crossing[k].wait_recv()
        place = out_ref.at[source, across]
        copy = remote(place, place, c_send.at[1, k], c_recv.at[1, k], {"tp": pair})
        copy.start()
        pairing.append(copy)

    pass_on(0)
    for k in range(1, n_ep):
        along[k - 1].wait_recv()
        pass_on(k)
        relay(k - 1)
    relay(n_ep - 1)
    for copy in pairing:
        copy.wait()
    for copy in crossing + along:
        copy.wait_send()
    own.wait()


def spread_rows(send_rows):
    n_ep = lax.axis_size("ep")
    n_tp = lax.axis_size("tp")
    if n_tp != 4:
        arrived = lax.all_to_all(send_rows, "ep", split_axis=0, concat_axis=0, tiled=True)
        return lax.all_gather(arrived, "tp", axis=1, tiled=True)
    _, part_len, width = send_rows.shape
    dma = pltpu.SemaphoreType.DMA
    arrived = pl.pallas_call(
        functools.partial(spread_kernel, n_ep, n_tp),
        out_shape=jax.ShapeDtypeStruct((n_ep, n_tp, part_len, width), send_rows.dtype),
        in_specs=[pl.BlockSpec(memory_space=pltpu.VMEM)],
        out_specs=pl.BlockSpec(memory_space=pltpu.VMEM),
        scratch_shapes=[
            dma,
            dma((n_ep,)),
            dma((n_ep,)),
            dma((n_ep,)),
            dma((n_ep,)),
            dma((2, n_ep)),
            dma((2, n_ep)),
        ],
        compiler_params=pltpu.CompilerParams(
            collective_id=0, has_side_effects=True, vmem_limit_bytes=16 * 2**20
        ),
        cost_estimate=pl.CostEstimate(flops=0, bytes_accessed=50_000_000, transcendentals=0),
    )(send_rows)
    return arrived.reshape(n_ep, n_tp * part_len, width)


def return_kernel(
    n_ep,
    n_tp,
    rows_ref,
    after_ref,
    out_ref,
    paired,
    leaving,
    crossed,
    final,
    c_send,
    c_recv,
    x_send,
    x_recv,
    z_send,
    z_recv,
):
    me, mine, pair, across = ring_peers(n_ep, n_tp)
    meet(me, pair, across, n_ep)
    width = out_ref.shape[2]
    pair_across = (pair + n_tp // 2) % n_tp

    def columns(quarter):
        return pl.ds(pl.multiple_of(quarter * width, width), width)

    order = list(range(1, n_ep)) + [0]
    pairing = {}
    for k in order:
        dest = (me + k) % n_ep
        for side, quarter in ((1, pair_across), (0, pair)):
            copy = remote(
                rows_ref.at[dest, :, columns(quarter)],
                paired.at[side, k],
                c_send.at[side, k],
                c_recv.at[side, k],
                {"tp": pair},
            )
            copy.start()
            pairing[side, k] = copy
    crossing = {}
    for k in order:
        dest = (me + k) % n_ep
        pairing[1, k].wait_recv()
        both = rows_ref[dest, :, columns(across)].astype(jnp.float32) + paired[1, k].astype(
            jnp.float32
        )
        leaving[k] = both.astype(leaving.dtype)
        copy = remote(leaving.at[k], crossed.at[k], x_send.at[k], x_recv.at[k], {"tp": across})
        copy.start()
        crossing[k] = copy
    along = []
    for k in order:
        dest = (me + k) % n_ep
        pairing[0, k].wait_recv()
        crossing[k].wait_recv()
        total = rows_ref[dest, :, columns(mine)].astype(jnp.float32) + paired[0, k].astype(
            jnp.float32
        )
        total = (total + crossed[k].astype(jnp.float32)).astype(out_ref.dtype)
        if k == 0:
            out_ref[me] = total
        else:
            final[k] = total
            copy = remote(final.at[k], out_ref.at[me], z_send.at[k], z_recv.at[k], {"ep": dest})
            copy.start()
            along.append(copy)
    for copy in along:
        copy.wait()
    for copy in list(pairing.values()) + list(crossing.values()):
        copy.wait_send()


def return_rows(partial_rows, after):
    n_ep = lax.axis_size("ep")
    n_tp = lax.axis_size("tp")
    if n_tp != 4:
        summed = lax.psum_scatter(partial_rows, "tp", scatter_dimension=2, tiled=True)
        return lax.all_to_all(summed, "ep", split_axis=0, concat_axis=0, tiled=True)
    _, row_cap, model_width = partial_rows.shape
    width = model_width // n_tp
    dma = pltpu.SemaphoreType.DMA
    kind = partial_rows.dtype
    return pl.pallas_call(
        functools.partial(return_kernel, n_ep, n_tp),
        out_shape=jax.ShapeDtypeStruct((n_ep, row_cap, width), kind),
        in_specs=[
            pl.BlockSpec(memory_space=pltpu.VMEM),
            pl.BlockSpec(memory_space=pl.ANY),
        ],
        out_specs=pl.BlockSpec(memory_space=pltpu.VMEM),
        scratch_shapes=[
            pltpu.VMEM((2, n_ep, row_cap, width), kind),
            pltpu.VMEM((n_ep, row_cap, width), kind),
            pltpu.VMEM((n_ep, row_cap, width), kind),
            pltpu.VMEM((n_ep, row_cap, width), kind),
            dma((2, n_ep)),
            dma((2, n_ep)),
            dma((n_ep,)),
            dma((n_ep,)),
            dma((n_ep,)),
            dma((n_ep,)),
        ],
        compiler_params=pltpu.CompilerParams(
            collective_id=1, has_side_effects=True, vmem_limit_bytes=20 * 2**20
        ),
        cost_estimate=pl.CostEstimate(flops=0, bytes_accessed=50_000_000, transcendentals=0),
    )(partial_rows, after)


def grouped_experts_half(
    expert_rows,
    expert_gain,
    routes,
    route_weight,
    gate_weight,
    up_weight,
    down_weight,
    mixer_part,
):
    n_tp = lax.axis_size("tp")
    n_ep = lax.axis_size("ep")
    span_rows, model_width = expert_rows.shape
    exp_dev = gate_weight.shape[0]
    capacity = n_tp * ((3 * (span_rows // n_tp) * TOP + 2 * EXPERTS - 1) // (2 * EXPERTS))
    row_cap = exp_dev * capacity // TOP
    part_len = row_cap // n_tp
    row_of, meta = route_plan(routes, route_weight, n_ep, exp_dev, row_cap)
    normed = head_norm(expert_rows, expert_gain).astype(jnp.bfloat16)
    wanted = jnp.arange(n_ep, dtype=jnp.int32)[:, None] * row_cap + (
        lax.axis_index("tp") * part_len + jnp.arange(part_len, dtype=jnp.int32)
    )
    select = (wanted.reshape(-1)[:, None] == row_of[None, :]).astype(jnp.bfloat16)
    send_rows = jnp.dot(
        select, jnp.concatenate([normed, meta], axis=1), preferred_element_type=jnp.float32
    ).astype(jnp.bfloat16)
    arrived = spread_rows(send_rows.reshape(n_ep, part_len, model_width + META))
    arrived, mixer_part = lax.optimization_barrier((arrived, mixer_part))
    notes = arrived[:, :, model_width : model_width + 8].astype(jnp.float32)
    slots = jnp.arange(exp_dev * capacity, dtype=jnp.float32)
    hits = []
    for j in range(TOP):
        local = notes[:, :, 2 * j]
        slot = jnp.where(local > 0, (local - 1) * capacity + notes[:, :, 2 * j + 1], -1.0)
        hits.append(slot[:, :, None] == slots)
    slot_rows = jnp.einsum(
        "nrq,nrd->nqd",
        (hits[0] | hits[1]).astype(jnp.bfloat16),
        arrived[:, :, :model_width],
        preferred_element_type=jnp.float32,
    ).astype(jnp.bfloat16)
    slot_rows = slot_rows.reshape(n_ep, exp_dev, capacity, model_width)
    gate_part = jnp.einsum(
        "nxcd,xdf->nxcf", slot_rows, gate_weight, preferred_element_type=jnp.float32
    )
    up_part = jnp.einsum("nxcd,xdf->nxcf", slot_rows, up_weight, preferred_element_type=jnp.float32)
    hidden = (jax.nn.silu(gate_part) * up_part).astype(jnp.bfloat16)
    down_part = jnp.einsum(
        "nxcf,xfd->nxcd", hidden, down_weight, preferred_element_type=jnp.float32
    ).astype(jnp.bfloat16)
    down_part = down_part.reshape(n_ep, exp_dev * capacity, model_width)
    partial_rows = 0.0
    for piece in range(2):
        weights = sum(
            jnp.where(hits[j], notes[:, :, 2 * TOP + 2 * j + piece][:, :, None], 0.0)
            for j in range(TOP)
        )
        partial_rows = partial_rows + jnp.einsum(
            "nrq,nqd->nrd",
            weights.astype(jnp.bfloat16),
            down_part,
            preferred_element_type=jnp.float32,
        )
    returned = return_rows(partial_rows.astype(jnp.bfloat16), mixer_part[:16, :128])
    returned = returned.reshape(n_ep * row_cap, model_width // n_tp)
    all_rows = jnp.arange(n_ep * row_cap, dtype=jnp.int32)
    return jnp.dot(
        (row_of[:, None] == all_rows[None, :]).astype(jnp.bfloat16),
        returned,
        preferred_element_type=jnp.float32,
    ).astype(jnp.bfloat16)


def on_device(
    queries,
    key_rows,
    value_rows,
    query_gain,
    key_gain,
    log_forget,
    out_weight,
    expert_rows,
    expert_gain,
    routes,
    route_weight,
    gate_weight,
    up_weight,
    down_weight,
):
    mixer_part = mixer_half(
        queries, key_rows, value_rows, query_gain, key_gain, log_forget, out_weight
    )
    expert_args = (
        expert_rows,
        expert_gain,
        routes,
        route_weight,
        gate_weight,
        up_weight,
        down_weight,
    )
    if gate_weight.shape[0] % GROUP_SIZE == 0:
        expert_out = grouped_experts_half(*expert_args, mixer_part)
    else:
        expert_out = experts_half(*expert_args)
    mixer_out = lax.psum_scatter(mixer_part, "tp", scatter_dimension=0, tiled=True)
    return (mixer_out, expert_out)


def solution(mesh):
    in_specs = (
        P(("grp", "ep"), "tp"),
        P(("grp", "ep"), "tp"),
        P(("grp", "ep"), "tp"),
        P(),
        P(),
        P("tp", "grp"),
        P("tp", None),
        P(("grp", "ep"), None),
        P(),
        P(None, ("grp", "ep")),
        P(None, ("grp", "ep")),
        P("ep", None, "tp"),
        P("ep", None, "tp"),
        P("ep", "tp", None),
    )
    out_specs = (P(("grp", "ep", "tp"), None), P(("grp", "ep"), "tp"))
    return jax.shard_map(
        on_device, mesh=mesh, in_specs=in_specs, out_specs=out_specs, check_vma=False
    )
```
